128 devices in a mesh: sp: 32 (over z, y, core), tp: 4 (over x).
Axes of the slice: x: 4, y: 4, z: 4, core: 2. Of those that a mesh axis runs over, the one named last changes fastest.
Arguments:
- queries: bfloat16 [6144, 1024], P('sp', 'tp'), may hold values from -0.75 to 0.75
- key_vectors: bfloat16 [6144, 1024], P('sp', 'tp'), may hold values from -0.75 to 0.75
- values_in: bfloat16 [6144, 2048], P('sp', 'tp'), may hold values from -0.75 to 0.75
- log_decay: float32 [6144, 1024], P('sp', 'tp'), may hold values from -1 to 0
- mixed_heads: bfloat16 [6144, 2048], P('sp', 'tp'), may hold values from -6 to 6
- out_proj: bfloat16 [2048, 2048], P('tp'), may hold values from -0.125 to 0.125
- layer_input: bfloat16 [6144, 2048], P('sp'), may hold values from -6 to 6
- cotangent: bfloat16 [6144, 2048], P('sp'), may hold values from -6 to 6
- routes: int32 [6144, 2], P('sp'), may hold values from 0 to 63, all different within a row; in each aligned block of 192 rows (0 to 191, 192 to 383, ...) at most 12 rows name the same one
- route_weight: float32 [6144, 2], P('sp'), may hold values from 0.25 to 2
- gate_weight: bfloat16 [64, 2048, 1024], P('sp', None, 'tp'), may hold values from -0.125 to 0.125
- up_weight: bfloat16 [64, 2048, 1024], P('sp', None, 'tp'), may hold values from -0.125 to 0.125
- down_weight: bfloat16 [64, 1024, 2048], P('sp', 'tp'), may hold values from -0.1875 to 0.1875
Outputs:
- grad_gate: float32 [64, 2048, 1024], P('sp', None, 'tp')
- grad_up: float32 [64, 2048, 1024], P('sp', None, 'tp')
- grad_down: float32 [64, 1024, 2048], P('sp', 'tp')
- grad_proj: float32 [2048, 2048], P('sp', 'tp')
- grad_query: float32 [6144, 1024], P('sp', 'tp')
- grad_key: float32 [6144, 1024], P('sp', 'tp')
- grad_value: float32 [6144, 2048], P('sp', 'tp')
- grad_decay: float32 [6144, 1024], P('sp', 'tp')
The draws below stay inside these ranges and needn't reach their ends.
Inputs may be any that keep to these rules, and one draw needn't show every extreme that they name: `routes`: in each aligned block of 192 tokens no expert is named by more than 12 pairs, and in some block one expert is named by exactly 12 pairs; the 2 experts of a token differ.
All inputs are finite; a program needn't handle non-finite values.
Results may differ from the reference program's by a relative error of at most 0.015.
Values may be sent and summed in bfloat16 or wider, within the bound.
A program may use at most 192 MiB of HBM per device.

```python
import math
import jax
import jax.numpy as jnp
import numpy as np
from jax import lax

D = 2048
HEADS = 8
DK = 128
DV = 256
FE = 1024
TOP = 2
TOK_DEV = 192
EXPERTS = 64
STREAM_LENGTH = 6144
CAP = 12
N_TP = 4


def draw_log_decay(key, part):
    lookup_entries = jax.random.split(key, 7)
    feature_total = HEADS * DK
    fast_share = 0.5
    fast = jax.random.bernoulli(lookup_entries[0], fast_share, (feature_total,))
    fast_rate = jnp.exp(jax.random.uniform(lookup_entries[1], (feature_total,), jnp.float32, jnp.log(1.0 / 50.0), jnp.log(1.0 / 30.0)))
    slow_rate = jnp.exp(jax.random.uniform(lookup_entries[2], (feature_total,), jnp.float32, jnp.log(0.05), jnp.log(0.25))) / STREAM_LENGTH
    rate = jnp.where(fast, fast_rate, slow_rate)
    blocks = STREAM_LENGTH // TOK_DEV
    block_factor = jnp.exp(jax.random.uniform(lookup_entries[3], (blocks, 1, 1), jnp.float32, -0.7, 0.7))
    rough = jnp.exp(jax.random.uniform(lookup_entries[4], (blocks, TOK_DEV, feature_total), jnp.float32, -0.4, 0.4))
    stable_mode = -(rate[None, None, :] * block_factor * rough).reshape(STREAM_LENGTH, feature_total)
    spike_location = jax.random.randint(lookup_entries[5], (3,), 0, STREAM_LENGTH)
    spike_surcharge = jax.random.uniform(lookup_entries[6], (feature_total,), jnp.float32, 0.2, 0.5)
    spike_indicator = jnp.any(jnp.arange(STREAM_LENGTH)[:, None] == spike_location[None, :], axis=1)
    return stable_mode + jnp.where(spike_indicator[:, None], jnp.log(1.0 - spike_surcharge)[None, :], 0.0)


def strengthened(entries, rng, source, target, shards_of, factor):
    owner, partner = [(jnp.arange(entries.shape[dim]) // (entries.shape[dim] // shards_of)).reshape([-1 if axis == dim else 1 for axis in range(entries.ndim)]) for dim in (source, target)]
    chosen = jax.random.permutation(rng, shards_of)[partner]
    strong = (owner == chosen) | (owner == (partner + shards_of // 2) % shards_of)
    return jnp.where(strong, factor * entries, entries)


def steps_of(key, shape, shards, smallest, high):
    def one(axis_at, shards_of):
        draws = jax.random.uniform(jax.random.fold_in(jax.random.fold_in(key, 6), axis_at), (shards_of,), jnp.float32, smallest / len(shards), high / len(shards))
        return jnp.repeat(jnp.exp(draws), shape[axis_at] // shards_of).reshape((-1,) + (1,) * (len(shape) - axis_at - 1))

    level = one(*shards[0])
    for cut in shards[1:]:
        level = level * one(*cut)
    return level


def deal_out(rng, own, number, rows, amount, top, bound, slope):
    ranking = jax.random.permutation(rng, amount)
    packed, common = shares(amount, rows * top, bound, slope, True), shares(amount, rows * top, bound, slope, False)
    places = jnp.arange(amount)

    def named(lengths, turn):
        used = int((lengths > 0).sum())
        fixed = max(1, used // 4)
        shifted = fixed + (places - fixed + turn * (used - fixed)) % max(1, amount - fixed)
        return jnp.zeros((amount,), jnp.int32).at[ranking[jnp.where(places < fixed, places, shifted)]].set(jnp.asarray(lengths, jnp.int32))

    lengths = jnp.where(number % 4 == 0, named(packed, number // 4), named(common, number - number // 4 - 1))
    mixed = jax.random.permutation(jax.random.fold_in(own, 3), amount)
    source_of, receiver = mixed[0:amount // 2 * 2:2], mixed[1:amount // 2 * 2:2]
    margin = jnp.minimum(lengths[source_of] - 1, bound - lengths[receiver]) // 2
    margin = jnp.where((source_of == ranking[0]) | (receiver == ranking[0]) | (lengths[receiver] == 0), 0, jnp.maximum(margin, 0))
    shifted = jax.random.randint(jax.random.fold_in(own, 4), (amount // 2,), 0, 1 << 20) % (margin + 1)
    lengths = lengths.at[source_of].add(-shifted).at[receiver].add(shifted)
    labels = jnp.searchsorted(jnp.cumsum(lengths), jnp.arange(rows * top), side="right").astype(jnp.int32)
    listing = labels.reshape(top, rows).T
    listing = listing[jax.random.permutation(jax.random.fold_in(own, 1), rows)]
    turn = jax.random.randint(jax.random.fold_in(own, 2), (rows, 1), 0, top)
    return jnp.take_along_axis(listing, (jnp.arange(top)[None, :] + turn) % top, axis=1)


def shares(number_of, total, limit, skew, full):
    portions = [(1 << 20) // math.isqrt(grade ** skew) + 1 for grade in range(1, number_of + 1)]
    largest = limit if full else min(limit, max(-(-total // number_of), total * portions[0] // sum(portions)))
    least = 1 if total - largest >= number_of - 1 else 0
    holding, spare = [largest] + [least] * (number_of - 1), total - largest - least * (number_of - 1)
    while spare > 0:
        free = [i for i in range(1, number_of) if holding[i] < largest] or [i for i in range(1, number_of) if holding[i] < limit]
        whole, left = sum([portions[i] for i in free]), spare
        for i in free:
            more = min(limit - holding[i], max(1, left * portions[i] // whole), spare)
            holding[i] = holding[i] + more
            spare = spare - more
    return np.array(holding)


def normal_values(key, shape, spread, limit, shards=(), kind=jnp.bfloat16):
    loudness = steps_of(key, shape, shards, -0.22, 0.18) if shards else 1.0
    values = jax.random.normal(key, shape, jnp.float32) * spread * loudness
    return jnp.minimum(jnp.maximum(values, -limit), limit).astype(kind)


def noise_with(key, dims, scale, reach, shards, heavy, kind=jnp.bfloat16):
    result = scale * jax.random.normal(key, dims, jnp.float32)
    if shards:
        result = result * steps_of(key, dims, shards, -0.22, 0.18)
    return jnp.clip(strengthened(result, jax.random.fold_in(key, 3), *heavy), -reach, reach).astype(kind)


def setup_inputs(seed: int = 0) -> dict:
    splits = jax.random.split(jax.random.key(seed), 14)
    queries = normal_values(splits[0], (STREAM_LENGTH, HEADS * DK), 0.125, 0.75, ((0, 32), (1, 4)))
    key_vectors = normal_values(splits[1], (STREAM_LENGTH, HEADS * DK), 0.125, 0.75, ((0, 32), (1, 4)))
    values_in = normal_values(splits[2], (STREAM_LENGTH, HEADS * DV), 0.125, 0.75, ((0, 32), (1, 4)))
    log_decay = draw_log_decay(jax.random.fold_in(splits[13], 71), 0)
    mixed_heads = normal_values(splits[4], (STREAM_LENGTH, HEADS * DV), 1.0, 6.0, ((0, 32), (1, 4)))
    out_proj = normal_values(splits[5], (HEADS * DV, D), (HEADS * DV) ** -0.5, 0.125, ((0, 4),))
    layer_input = normal_values(splits[6], (STREAM_LENGTH, D), 1.0, 6.0, ((0, 32),))
    cotangent = noise_with(splits[7], (STREAM_LENGTH, D), 1.0, 6.0, ((0, 32),), (0, 1, 32, 2.75))
    routes_keys = jax.random.split(jax.random.fold_in(splits[8], 1), STREAM_LENGTH // TOK_DEV)
    routes_turns = jax.random.permutation(jax.random.fold_in(splits[8], 3), STREAM_LENGTH // TOK_DEV)
    routes = jax.vmap(lambda own, number: deal_out(jax.random.fold_in(splits[8], 2), own, number, TOK_DEV, EXPERTS, TOP, CAP, 2))(routes_keys, routes_turns).reshape((STREAM_LENGTH, TOP))
    route_weight = jnp.clip(jnp.exp(math.log(2.0) - 2.0794415 * jax.random.uniform(splits[9], (STREAM_LENGTH, TOP), jnp.float32) ** steps_of(splits[9], (STREAM_LENGTH, TOP), ((0, 32),), -0.2, 0.2)), 0.25, 2.0)
    gate_weight = normal_values(splits[10], (EXPERTS, D, FE), D ** -0.5, 0.125, ((0, 32), (2, 4)))
    up_weight = normal_values(splits[11], (EXPERTS, D, FE), D ** -0.5, 0.125, ((0, 32), (2, 4)))
    down_weight = normal_values(splits[12], (EXPERTS, FE, D), FE ** -0.5, 0.1875, ((0, 32), (1, 4)))
    return dict(queries=queries, key_vectors=key_vectors, values_in=values_in, log_decay=log_decay, mixed_heads=mixed_heads, out_proj=out_proj, layer_input=layer_input, cotangent=cotangent, routes=routes, route_weight=route_weight, gate_weight=gate_weight, up_weight=up_weight, down_weight=down_weight)


def local_parts(query_f, key_f, grad_f, pair, decays):
    highest = lax.Precision.HIGHEST
    sigma = query_f.shape[2] ** -0.5
    length = query_f.shape[0]
    cum = jnp.cumsum(decays, axis=0)
    total = cum[-1]
    middle = 0.5 * total
    rise = jnp.exp(cum - middle)
    fall = jnp.exp(middle - cum)
    position = jnp.arange(length, dtype=jnp.int32)
    lower = (position[:, None] >= position[None, :])[None]
    score_fwd = jnp.where(lower, jnp.einsum("thc,shc->hts", query_f * rise, key_f * fall, precision=highest), 0.0) * sigma
    score_bwd = jnp.where(lower, 0.0, jnp.einsum("thc,shc->hts", query_f * fall, key_f * rise, precision=highest)) * sigma
    pair_fwd = jnp.where(lower, pair, 0.0)
    pair_bwd = jnp.where(lower, 0.0, pair)
    query_fwd = sigma * rise * jnp.einsum("hts,shc->thc", pair_fwd, key_f * fall, precision=highest)
    query_bwd = sigma * fall * jnp.einsum("hts,shc->thc", pair_bwd, key_f * rise, precision=highest)
    key_fwd = sigma * fall * jnp.einsum("hts,thc->shc", pair_fwd, query_f * rise, precision=highest)
    key_bwd = sigma * rise * jnp.einsum("hts,thc->shc", pair_bwd, query_f * fall, precision=highest)
    value_grad = jnp.einsum("hts,thv->shv", score_fwd + score_bwd, grad_f, precision=highest)
    return query_fwd, query_bwd, key_fwd, key_bwd, value_grad, cum, total


def state_terms(query_f, key_f, value_f, grad_f, cum, total):
    highest = lax.Precision.HIGHEST
    head_part = jnp.exp(cum)
    tail = jnp.exp(total - cum)
    kv_fwd = jnp.einsum("shc,shv->hcv", key_f * tail, value_f, precision=highest)
    qo_bwd = jnp.einsum("thc,thv->hcv", query_f * tail, grad_f, precision=highest)
    qo_fwd = jnp.einsum("thc,thv->hcv", query_f * head_part, grad_f, precision=highest)
    kv_bwd = jnp.einsum("shc,shv->hcv", key_f * head_part, value_f, precision=highest)
    return jnp.exp(total), kv_fwd, qo_bwd, qo_fwd, kv_bwd


def carried(parts, states, query_f, key_f, value_f, grad_f):
    highest = lax.Precision.HIGHEST
    sigma = query_f.shape[2] ** -0.5
    query_fwd, query_bwd, key_fwd, key_bwd, value_grad, cum, total = parts
    kv_low, qo_low, qo_high, kv_high = states
    head_part = jnp.exp(cum)
    tail = jnp.exp(total - cum)
    query_fwd = query_fwd + sigma * head_part * jnp.einsum("thv,hcv->thc", grad_f, kv_low, precision=highest)
    query_bwd = query_bwd + sigma * tail * jnp.einsum("thv,hcv->thc", grad_f, kv_high, precision=highest)
    key_fwd = key_fwd + sigma * tail * jnp.einsum("shv,hcv->shc", value_f, qo_high, precision=highest)
    key_bwd = key_bwd + sigma * head_part * jnp.einsum("shv,hcv->shc", value_f, qo_low, precision=highest)
    value_grad = value_grad + sigma * (jnp.einsum("shc,hcv->shv", key_f * tail, qo_high, precision=highest)
                                       + jnp.einsum("shc,hcv->shv", key_f * head_part, qo_low, precision=highest))
    grad_cum = query_f * (query_fwd - query_bwd) - key_f * (key_fwd - key_bwd)
    return query_fwd + query_bwd, key_fwd + key_bwd, value_grad, grad_cum


def carry_step(carry, inputs):
    decay_all, first_term, second_term = inputs
    grown = (decay_all[..., None] * carry[0] + first_term, decay_all[..., None] * carry[1] + second_term)
    return grown, carry


def expert_grads(inputs):
    rows, cots, weights, gate_w, up_w, down_w = inputs
    pre_gate = jnp.dot(rows, gate_w, preferred_element_type=jnp.float32)
    pre_up = jnp.dot(rows, up_w, preferred_element_type=jnp.float32)
    weighted = (weights[:, None] * cots.astype(jnp.float32)).astype(jnp.bfloat16)
    d_act = jnp.dot(weighted, down_w.T, preferred_element_type=jnp.float32)
    sigmoid_gate = jax.nn.sigmoid(pre_gate)
    silu_gate = pre_gate * sigmoid_gate
    act = (silu_gate * pre_up).astype(jnp.bfloat16)
    d_gate = (d_act * pre_up * sigmoid_gate * (1.0 + pre_gate * (1.0 - sigmoid_gate))).astype(jnp.bfloat16)
    d_up = (d_act * silu_gate).astype(jnp.bfloat16)
    grad_down = jnp.dot(act.T, weighted, preferred_element_type=jnp.float32)
    grad_gate = jnp.dot(rows.T, d_gate, preferred_element_type=jnp.float32)
    grad_up = jnp.dot(rows.T, d_up, preferred_element_type=jnp.float32)
    part_width = FE // N_TP
    parts = jnp.einsum("rpf,pfd->rpd", d_gate.reshape(-1, N_TP, part_width).astype(jnp.float32),
                       gate_w.T.reshape(N_TP, part_width, D).astype(jnp.float32))
    parts = parts + jnp.einsum("rpf,pfd->rpd", d_up.reshape(-1, N_TP, part_width).astype(jnp.float32),
                               up_w.T.reshape(N_TP, part_width, D).astype(jnp.float32))
    rounded = lax.optimization_barrier(parts.astype(jnp.bfloat16))
    row_grad = jnp.sum(rounded.astype(jnp.float32), axis=1).astype(jnp.bfloat16)
    return grad_gate, grad_up, grad_down, row_grad


def reference(queries, key_vectors, values_in, log_decay, mixed_heads, out_proj, layer_input, cotangent,
              routes, route_weight, gate_weight, up_weight, down_weight):
    blocks = STREAM_LENGTH // TOK_DEV
    rows_all = blocks * CAP
    flat_route = routes.reshape(blocks, TOK_DEV * TOP)
    onehot = (flat_route[:, :, None] == jnp.arange(EXPERTS, dtype=jnp.int32)[None, None, :]).astype(jnp.int32)
    rank = jnp.sum((jnp.cumsum(onehot, axis=1) - onehot) * onehot, axis=2)
    block_id = jnp.arange(blocks, dtype=jnp.int32)[:, None]
    place = (flat_route * rows_all + block_id * CAP + rank).reshape(-1).astype(jnp.int32)
    token_id = jnp.arange(STREAM_LENGTH * TOP, dtype=jnp.int32) // TOP
    slot_token = jnp.zeros((EXPERTS * rows_all,), jnp.int32).at[place].set(token_id)
    filled = jnp.zeros((EXPERTS * rows_all,), jnp.float32).at[place].set(1.0)
    slot_weight = jnp.zeros((EXPERTS * rows_all,), jnp.float32).at[place].set(route_weight.reshape(-1))
    expert_rows = (layer_input[slot_token].astype(jnp.float32) * filled[:, None]).astype(jnp.bfloat16)
    expert_cot = (cotangent[slot_token].astype(jnp.float32) * filled[:, None]).astype(jnp.bfloat16)
    grad_gate, grad_up, grad_down, row_grad = lax.map(expert_grads, (
        expert_rows.reshape(EXPERTS, rows_all, D), expert_cot.reshape(EXPERTS, rows_all, D),
        slot_weight.reshape(EXPERTS, rows_all), gate_weight, up_weight, down_weight))
    back = row_grad.reshape(EXPERTS * rows_all, D)[place].reshape(STREAM_LENGTH, TOP, D)
    token_grad = (cotangent.astype(jnp.float32) + jnp.sum(back.astype(jnp.float32), axis=1)).astype(jnp.bfloat16)
    grad_proj = jnp.dot(token_grad.T, mixed_heads, preferred_element_type=jnp.float32)
    head_grad = jnp.dot(token_grad, out_proj.T, preferred_element_type=jnp.float32)

    highest = lax.Precision.HIGHEST
    query_f = queries.astype(jnp.float32).reshape(blocks, TOK_DEV, HEADS, DK)
    key_f = key_vectors.astype(jnp.float32).reshape(blocks, TOK_DEV, HEADS, DK)
    value_f = values_in.astype(jnp.float32).reshape(blocks, TOK_DEV, HEADS, DV)
    grad_f = head_grad.reshape(blocks, TOK_DEV, HEADS, DV)
    decays = log_decay.reshape(blocks, TOK_DEV, HEADS, DK)
    pair = jnp.einsum("bthv,bshv->bhts", grad_f, value_f, precision=highest)
    parts = jax.vmap(local_parts)(query_f, key_f, grad_f, pair, decays)
    terms = jax.vmap(state_terms)(query_f, key_f, value_f, grad_f, parts[5], parts[6])
    zeros = jnp.zeros((HEADS, DK, DV), jnp.float32)
    _, low = lax.scan(carry_step, (zeros, zeros), (terms[0], terms[1], terms[2]))
    _, high = lax.scan(carry_step, (zeros, zeros), (terms[0], terms[3], terms[4]), reverse=True)
    query_grad, key_grad, value_grad, grad_cum = jax.vmap(carried)(
        parts, (low[0], low[1], high[0], high[1]), query_f, key_f, value_f, grad_f)
    grad_cum = grad_cum.reshape(STREAM_LENGTH, HEADS * DK)
    grad_decay = jnp.flip(jnp.cumsum(jnp.flip(grad_cum, 0), axis=0), 0)
    return (grad_gate, grad_up, grad_down, grad_proj, query_grad.reshape(STREAM_LENGTH, HEADS * DK),
            key_grad.reshape(STREAM_LENGTH, HEADS * DK), value_grad.reshape(STREAM_LENGTH, HEADS * DV), grad_decay)
```

```python
import functools
import jax
import jax.numpy as jnp
from jax import lax
from jax.experimental import pallas as pl
from jax.experimental.pallas import tpu as pltpu
from jax.sharding import PartitionSpec as P

DK = 128
DV = 256
TOK = 192
SP = 32
TP = 4
CAP = 12
QW = 512
F32 = jnp.float32
BF16 = jnp.bfloat16
VM = pltpu.VMEM
CHIP_OFF = (
    (1, 0), (0, 1), (3, 0), (0, 3), (1, 1), (3, 3), (2, 0), (0, 2),
    (1, 3), (3, 1), (2, 1), (1, 2), (2, 3), (3, 2), (2, 2),
)
OFFS = ((0, 0, 1),) + tuple((dy, dz, dc) for dy, dz in CHIP_OFF for dc in (0, 1))


def moved(me, off, sign):
    dy, dz, dc = off
    core, y, z = lax.rem(me, 2), lax.rem(me // 2, 4), me // 8
    if sign < 0:
        dy, dz = (4 - dy) % 4, (4 - dz) % 4
    core = core if dc == 0 else 1 - core
    y = y if dy == 0 else lax.rem(y + dy, 4)
    z = z if dz == 0 else lax.rem(z + dz, 4)
    return (z * 4 + y) * 2 + core


def dot(a, b, dims, precision=None):
    return lax.dot_general(a, b, (dims, ((), ())), preferred_element_type=F32, precision=precision)


NN = ((1,), (0,))
NT = ((1,), (1,))
TN = ((0,), (0,))


def prep_kernel(routes_ref, weight_ref, rows_ref, cot_ref, place_ref, send_ref):
    mx = lax.axis_index("tp")
    experts = 2 * SP
    e_row = lax.broadcasted_iota(jnp.int32, (experts, TOK), 0)
    r0 = routes_ref[0:1, :]
    r1 = routes_ref[1:2, :]
    oh0 = jnp.where(e_row == r0, 1.0, 0.0)
    oh1 = jnp.where(e_row == r1, 1.0, 0.0)
    before = jnp.where(
        lax.broadcasted_iota(jnp.int32, (TOK, TOK), 0)
        < lax.broadcasted_iota(jnp.int32, (TOK, TOK), 1), 1.0, 0.0,
    )
    earlier = dot((oh0 + oh1).astype(BF16), before.astype(BF16), NN)
    slots = []
    for route, oh in ((r0, oh0), (r1, oh1)):
        rank = jnp.sum(oh * earlier, axis=0, keepdims=True).astype(jnp.int32)
        dest, local = route >> 1, route & 1
        pos = jnp.where(local == 0, rank, jnp.where(rank < 8, 16 + rank, 4 + rank))
        slots.append((pos >> 3) * (SP * 8) + dest * 8 + (pos & 7))
    slot_row = lax.broadcasted_iota(jnp.int32, (24 * SP, TOK), 0)
    hit0, hit1 = slot_row == slots[0], slot_row == slots[1]
    place = jnp.where(hit0 | hit1, 1.0, 0.0).astype(BF16)
    place_ref[...] = place
    weight = jnp.sum(
        jnp.where(hit0, weight_ref[0:1, :], 0.0) + jnp.where(hit1, weight_ref[1:2, :], 0.0),
        axis=1, keepdims=True,
    )
    for half in range(2):
        quarter = lax.rem(mx + 2 * half, TP)
        cols = pl.ds(pl.multiple_of(quarter * QW, QW), QW)
        send_ref[half, 0] = dot(place, rows_ref[:, cols], NN).astype(BF16)
        send_ref[half, 1] = (dot(place, cot_ref[:, cols], NN) * weight).astype(BF16)


def prep(routes_t, weight_t, rows, cot):
    return pl.pallas_call(
        prep_kernel,
        name="prep",
        out_shape=(
            jax.ShapeDtypeStruct((24 * SP, TOK), BF16),
            jax.ShapeDtypeStruct((2, 2, 24 * SP, QW), BF16),
        ),
        in_specs=[pl.BlockSpec(memory_space=VM)] * 4,
        out_specs=(pl.BlockSpec(memory_space=VM),) * 2,
        compiler_params=pltpu.CompilerParams(vmem_limit_bytes=32 << 20),
    )(routes_t, weight_t, rows, cot)


def dispatch_kernel(send_ref, out_ref, ssem, rsem, fsem, gsem, lsem):
    me, mx = lax.axis_index("sp"), lax.axis_index("tp")
    quarters = (mx, lax.rem(mx + 2, TP))
    sides = (lax.rem(mx + 1, TP), lax.rem(mx + 3, TP))
    barrier = pltpu.get_barrier_semaphore()
    for off in OFFS:
        pl.semaphore_signal(barrier, inc=1, device_id={"sp": moved(me, off, 1)})
    for side in sides:
        pl.semaphore_signal(barrier, inc=1, device_id={"tp": side})
    pl.semaphore_wait(barrier, len(OFFS) + 2)

    def plane(half, i):
        peer = moved(me, OFFS[i], 1)
        return pltpu.make_async_remote_copy(
            src_ref=send_ref.at[half, :, :, peer],
            dst_ref=out_ref.at[:, quarters[half], :, me],
            send_sem=ssem.at[half, i], recv_sem=rsem.at[half, i], device_id={"sp": peer},
        )

    def forward(way, i, src):
        return pltpu.make_async_remote_copy(
            src_ref=out_ref.at[:, quarters[0], :, src],
            dst_ref=out_ref.at[:, quarters[0], :, src],
            send_sem=fsem.at[way, i], recv_sem=gsem.at[way, i], device_id={"tp": sides[way]},
        )

    own = [
        pltpu.make_async_copy(
            send_ref.at[half, :, :, me], out_ref.at[:, quarters[half], :, me], lsem.at[half]
        )
        for half in range(2)
    ]
    for half in range(2):
        own[half].start()
    for half in range(2):
        for i in range(len(OFFS)):
            plane(half, i).start()
    own[0].wait()
    for way in range(2):
        forward(way, len(OFFS), me).start()
    for i, off in enumerate(OFFS):
        plane(0, i).wait_recv()
        for way in range(2):
            forward(way, i, moved(me, off, -1)).start()
    own[1].wait()
    for i in range(len(OFFS)):
        plane(1, i).wait_recv()
    for i in range(len(OFFS)):
        plane(0, i).wait_send()
        plane(1, i).wait_send()
    for i in range(len(OFFS) + 1):
        src = me if i == len(OFFS) else moved(me, OFFS[i], -1)
        for way in range(2):
            forward(way, i, src).wait()


def dispatch(send):
    n = len(OFFS)
    return pl.pallas_call(
        dispatch_kernel,
        name="dispatch",
        out_shape=jax.ShapeDtypeStruct((2, TP, 3, SP, 8, QW), BF16),
        in_specs=[pl.BlockSpec(memory_space=VM)],
        out_specs=pl.BlockSpec(memory_space=VM),
        scratch_shapes=[
            pltpu.SemaphoreType.DMA((2, n)),
            pltpu.SemaphoreType.DMA((2, n)),
            pltpu.SemaphoreType.DMA((2, n + 1)),
            pltpu.SemaphoreType.DMA((2, n + 1)),
            pltpu.SemaphoreType.DMA((2,)),
        ],
        compiler_params=pltpu.CompilerParams(
            collective_id=1, has_side_effects=True, vmem_limit_bytes=24 << 20
        ),
    )(send)


def expert_kernel(rows_ref, gate_ref, up_ref, down_ref, part_ref, act_ref, dg_ref, du_ref):
    for e in range(2):
        rows = pl.ds(256 * e, 512)
        pre_gate = pre_up = d_act = None
        for q in range(TP):
            cols = pl.ds(q * QW, QW)
            x, w = rows_ref[0, q, rows], rows_ref[1, q, rows]
            terms = (
                dot(x, gate_ref[e, cols], NN),
                dot(x, up_ref[e, cols], NN),
                dot(w, down_ref[e, :, cols], NT),
            )
            if q == 0:
                pre_gate, pre_up, d_act = terms
            else:
                pre_gate, pre_up, d_act = pre_gate + terms[0], pre_up + terms[1], d_act + terms[2]
        row = lax.broadcasted_iota(jnp.int32, (512, 256), 0)
        if e == 0:
            mine = (row < 256) | ((row & 7) < 4)
        else:
            mine = (row >= 256) | ((row & 7) >= 4)
        sig = jax.nn.sigmoid(pre_gate)
        silu = pre_gate * sig
        act_ref[e] = jnp.where(mine, silu * pre_up, 0.0).astype(BF16)
        dg = jnp.where(mine, d_act * pre_up * sig * (1.0 + pre_gate * (1.0 - sig)), 0.0).astype(BF16)
        du = jnp.where(mine, d_act * silu, 0.0).astype(BF16)
        dg_ref[e] = dg
        du_ref[e] = du
        for q in range(TP):
            cols = pl.ds(q * QW, QW)
            part = dot(dg, gate_ref[e, cols], NT) + dot(du, up_ref[e, cols], NT)
            if e == 0:
                part_ref[q, 0:512] = part.astype(BF16)
            else:
                part_ref[q, 256:512] = (part_ref[q, 256:512].astype(F32) + part[:256]).astype(BF16)
                part_ref[q, 512:768] = part[256:].astype(BF16)


def experts(rows, gate, up, down):
    hidden = jax.ShapeDtypeStruct((2, 512, 256), BF16)
    return pl.pallas_call(
        expert_kernel,
        name="experts",
        out_shape=(jax.ShapeDtypeStruct((TP, 24 * SP, QW), BF16), hidden, hidden, hidden),
        in_specs=[pl.BlockSpec(memory_space=VM)] * 4,
        out_specs=(pl.BlockSpec(memory_space=VM),) * 4,
        compiler_params=pltpu.CompilerParams(vmem_limit_bytes=48 << 20),
    )(rows, gate, up, down)


def weight_grad_kernel(rows_ref, act_ref, dg_ref, du_ref, gg_ref, gu_ref, gd_ref):
    rows = pl.ds(pl.multiple_of(pl.program_id(1) * 256, 256), 512)
    x, w = rows_ref[0, 0, rows], rows_ref[1, 0, rows]
    gg_ref[0] = dot(x, dg_ref[0], TN)
    gu_ref[0] = dot(x, du_ref[0], TN)
    gd_ref[0] = dot(act_ref[0], w, TN)


def weight_grads(rows, act, dg, du):
    hidden = pl.BlockSpec((1, 512, 256), lambda q, e: (e, 0, 0))
    wide = pl.BlockSpec((1, QW, 256), lambda q, e: (e, q, 0))
    return pl.pallas_call(
        weight_grad_kernel,
        name="weight_grads",
        grid=(TP, 2),
        out_shape=(
            jax.ShapeDtypeStruct((2, 2048, 256), F32),
            jax.ShapeDtypeStruct((2, 2048, 256), F32),
            jax.ShapeDtypeStruct((2, 256, 2048), F32),
        ),
        in_specs=[
            pl.BlockSpec((2, 1, 24 * SP, QW), lambda q, e: (0, q, 0, 0)), hidden, hidden, hidden,
        ],
        out_specs=(wide, wide, pl.BlockSpec((1, 256, QW), lambda q, e: (e, 0, q))),
        compiler_params=pltpu.CompilerParams(vmem_limit_bytes=48 << 20),
    )(rows, act, dg, du)


def heads(x, width):
    return x.reshape(x.shape[0], 2, width)


def exchange(x):
    return lax.all_to_all(x, "sp", split_axis=0, concat_axis=0, tiled=True)


def scan_states(decay, first, second, backward):
    n = first.shape[1] * 2 // SP
    both = jnp.stack([first, second], axis=0).reshape(2, SP, n, DK).transpose(1, 0, 2, 3)
    got = exchange(both.astype(BF16)).astype(F32)
    head = lax.axis_index("sp") // (SP // 2)
    d = lax.dynamic_index_in_dim(decay, head, 1, keepdims=False)
    acc = jnp.zeros_like(got[0])
    outs = [None] * SP
    for s in (range(SP - 1, -1, -1) if backward else range(SP)):
        outs[s] = acc
        acc = d[s][None, None, :] * acc + got[s]
    back = exchange(jnp.stack(outs).astype(BF16)).astype(F32)
    back = back.transpose(1, 0, 2, 3).reshape(2, 2, DV, DK)
    return back[0], back[1]


def body(
    queries, key_vectors, values_in, log_decay, mixed_heads, out_proj, layer_input, cotangent,
    routes, route_weight, gate_weight, up_weight, down_weight,
):
    mx = lax.axis_index("tp")
    place, send = prep(routes.T, route_weight.T, layer_input, cotangent)
    got = dispatch(send.reshape(2, 2, 3, SP, 8, QW)).reshape(2, TP, 24 * SP, QW)
    part, act, dg, du = experts(got, gate_weight, up_weight, down_weight)
    grad_gate, grad_up, grad_down = weight_grads(got, act, dg, du)
    mine = lax.psum_scatter(part, "tp", scatter_dimension=0, tiled=True)
    back = lax.all_to_all(
        mine.reshape(3, SP, 8, QW), "sp", split_axis=1, concat_axis=1, tiled=True
    ).reshape(24 * SP, QW)
    own_cot = lax.dynamic_slice_in_dim(cotangent, mx * QW, QW, 1)
    token_part = (own_cot.astype(F32) + dot(place, back, TN)).astype(BF16)
    token_grad = lax.all_gather(token_part, "tp", axis=1, tiled=True)
    grad_proj = lax.psum_scatter(
        dot(token_grad, mixed_heads, TN), "sp", scatter_dimension=0, tiled=True
    )
    sigma = DK ** (-0.5)
    grad_f = heads(dot(token_grad, out_proj, NT), DV)
    q, k, v = heads(queries, DK).astype(F32), heads(key_vectors, DK).astype(F32), heads(values_in, DV)
    t_row = lax.broadcasted_iota(jnp.int32, (TOK, TOK), 0)
    t_col = lax.broadcasted_iota(jnp.int32, (TOK, TOK), 1)
    lower = t_row >= t_col
    cum = heads(dot(lower.astype(F32), log_decay, NN, lax.Precision.HIGHEST), DK)
    total = cum[-1]
    rise, fall = jnp.exp(cum - 0.5 * total), jnp.exp(0.5 * total - cum)
    head, tail = jnp.exp(cum), jnp.exp(total - cum)
    decay = lax.all_gather(jnp.exp(total), "sp")

    def mm(eq, a, b):
        return jnp.einsum(eq, a.astype(BF16), b.astype(BF16), preferred_element_type=F32)

    qr, qf, kr, kf = q * rise, q * fall, k * rise, k * fall
    qh, qt, kh, kt = q * head, q * tail, k * head, k * tail
    score = sigma * (
        jnp.where(lower, mm("thc,shc->hts", qr, kf), 0.0) + jnp.where(lower, 0.0, mm("thc,shc->hts", qf, kr))
    )
    pair = mm("thv,shv->hts", grad_f, v)
    pair_fwd, pair_bwd = jnp.where(lower, pair, 0.0), jnp.where(lower, 0.0, pair)
    kv_fwd, kv_bwd = mm("shv,shc->hvc", v, kt), mm("shv,shc->hvc", v, kh)
    qo_bwd, qo_fwd = mm("thv,thc->hvc", grad_f, qt), mm("thv,thc->hvc", grad_f, qh)
    kv_low, qo_low = scan_states(decay, kv_fwd, qo_bwd, False)
    qo_high, kv_high = scan_states(decay, qo_fwd, kv_bwd, True)
    q_fwd = sigma * (rise * mm("hts,shc->thc", pair_fwd, kf) + head * mm("thv,hvc->thc", grad_f, kv_low))
    q_bwd = sigma * (fall * mm("hts,shc->thc", pair_bwd, kr) + tail * mm("thv,hvc->thc", grad_f, kv_high))
    k_fwd = sigma * (fall * mm("hts,thc->shc", pair_fwd, qr) + tail * mm("shv,hvc->shc", v, qo_high))
    k_bwd = sigma * (rise * mm("hts,thc->shc", pair_bwd, qf) + head * mm("shv,hvc->shc", v, qo_low))
    value_grad = mm("hts,thv->shv", score, grad_f) + sigma * (
        mm("shc,hvc->shv", kt, qo_high) + mm("shc,hvc->shv", kh, qo_low)
    )
    grad_cum = (q * (q_fwd - q_bwd) - k * (k_fwd - k_bwd)).reshape(TOK, 2 * DK)
    d_own = jnp.exp(total)[:, None, :]
    beyond = sigma * jnp.sum(
        (d_own * kv_low + kv_fwd) * qo_high + (d_own * qo_low + qo_bwd) * kv_high, axis=1
    ).reshape(1, 2 * DK)
    upper = (t_row <= t_col).astype(F32)
    grad_decay = dot(upper, grad_cum, NN, lax.Precision.HIGHEST) + beyond
    return (
        grad_gate, grad_up, grad_down, grad_proj,
        (q_fwd + q_bwd).reshape(TOK, 2 * DK), (k_fwd + k_bwd).reshape(TOK, 2 * DK),
        value_grad.reshape(TOK, 2 * DV), grad_decay,
    )


def solution(mesh):
    return jax.shard_map(
        body,
        mesh=mesh,
        in_specs=(
            P("sp", "tp"), P("sp", "tp"), P("sp", "tp"), P("sp", "tp"), P("sp", "tp"),
            P("tp", None), P("sp", None), P("sp", None), P("sp", None), P("sp", None),
            P("sp", None, "tp"), P("sp", None, "tp"), P("sp", "tp", None),
        ),
        out_specs=(
            P("sp", None, "tp"), P("sp", None, "tp"), P("sp", "tp", None),
            P("sp", "tp"), P("sp", "tp"), P("sp", "tp"), P("sp", "tp"), P("sp", "tp"),
        ),
        check_vma=False,
    )
```

```python
import functools
import jax
import jax.numpy as jnp
from jax import lax
from jax.experimental import pallas as pl
from jax.experimental.pallas import tpu as pltpu
from jax.sharding import PartitionSpec as P

DK = 128
DV = 256
TOK = 192
SP = 32
TP = 4
CAP = 12
QW = 512
F32 = jnp.float32
BF16 = jnp.bfloat16
VM = pltpu.VMEM
CHIP_OFF = (
    (1, 0), (0, 1), (3, 0), (0, 3), (1, 1), (3, 3), (2, 0), (0, 2),
    (1, 3), (3, 1), (2, 1), (1, 2), (2, 3), (3, 2), (2, 2),
)
OFFS = ((0, 0, 1),) + tuple((dy, dz, dc) for dy, dz in CHIP_OFF for dc in (0, 1))


def moved(me, off, sign):
    dy, dz, dc = off
    core, y, z = lax.rem(me, 2), lax.rem(me // 2, 4), me // 8
    if sign < 0:
        dy, dz = (4 - dy) % 4, (4 - dz) % 4
    core = core if dc == 0 else 1 - core
    y = y if dy == 0 else lax.rem(y + dy, 4)
    z = z if dz == 0 else lax.rem(z + dz, 4)
    return (z * 4 + y) * 2 + core


def dot(a, b, dims, precision=None):
    return lax.dot_general(a, b, (dims, ((), ())), preferred_element_type=F32, precision=precision)


def lower_mask():
    row = lax.broadcasted_iota(jnp.int32, (TOK, TOK), 0)
    return row >= lax.broadcasted_iota(jnp.int32, (TOK, TOK), 1)


SIGMA = DK ** (-0.5)
RISE, FALL, HEAD, TAIL = 0, 1, 2, 3
NN = ((1,), (0,))
NT = ((1,), (1,))
TN = ((0,), (0,))


def prep_kernel(routes_ref, weight_ref, rows_ref, cot_ref, place_ref, send_ref):
    mx = lax.axis_index("tp")
    experts = 2 * SP
    e_row = lax.broadcasted_iota(jnp.int32, (experts, TOK), 0)
    r0 = routes_ref[0:1, :]
    r1 = routes_ref[1:2, :]
    oh0 = jnp.where(e_row == r0, 1.0, 0.0)
    oh1 = jnp.where(e_row == r1, 1.0, 0.0)
    before = jnp.where(
        lax.broadcasted_iota(jnp.int32, (TOK, TOK), 0)
        < lax.broadcasted_iota(jnp.int32, (TOK, TOK), 1), 1.0, 0.0,
    )
    earlier = dot((oh0 + oh1).astype(BF16), before.astype(BF16), NN)
    slots = []
    for route, oh in ((r0, oh0), (r1, oh1)):
        rank = jnp.sum(oh * earlier, axis=0, keepdims=True).astype(jnp.int32)
        dest, local = route >> 1, route & 1
        pos = jnp.where(local == 0, rank, jnp.where(rank < 8, 16 + rank, 4 + rank))
        slots.append((pos >> 3) * (SP * 8) + dest * 8 + (pos & 7))
    slot_row = lax.broadcasted_iota(jnp.int32, (24 * SP, TOK), 0)
    hit0, hit1 = slot_row == slots[0], slot_row == slots[1]
    place = jnp.where(hit0 | hit1, 1.0, 0.0).astype(BF16)
    place_ref[...] = place
    weight = jnp.sum(
        jnp.where(hit0, weight_ref[0:1, :], 0.0) + jnp.where(hit1, weight_ref[1:2, :], 0.0),
        axis=1, keepdims=True,
    )
    for half in range(2):
        quarter = lax.rem(mx + 2 * half, TP)
        cols = pl.ds(pl.multiple_of(quarter * QW, QW), QW)
        send_ref[half, 0] = dot(place, rows_ref[:, cols], NN).astype(BF16)
        send_ref[half, 1] = (dot(place, cot_ref[:, cols], NN) * weight).astype(BF16)


def prep(routes_t, weight_t, rows, cot):
    return pl.pallas_call(
        prep_kernel,
        name="prep",
        out_shape=(
            jax.ShapeDtypeStruct((24 * SP, TOK), BF16),
            jax.ShapeDtypeStruct((2, 2, 24 * SP, QW), BF16),
        ),
        in_specs=[pl.BlockSpec(memory_space=VM)] * 4,
        out_specs=(pl.BlockSpec(memory_space=VM),) * 2,
        compiler_params=pltpu.CompilerParams(vmem_limit_bytes=32 << 20),
    )(routes_t, weight_t, rows, cot)


def dispatch_kernel(
    send_ref, q_ref, k_ref, v_ref, decay_ref,
    out_ref, scale_ref, scaled_ref, score_ref, kv_ref, kvb_ref, total_ref,
    ssem, rsem, fsem, gsem, lsem,
):
    me, mx = lax.axis_index("sp"), lax.axis_index("tp")
    quarters = (mx, lax.rem(mx + 2, TP))
    sides = (lax.rem(mx + 1, TP), lax.rem(mx + 3, TP))
    barrier = pltpu.get_barrier_semaphore()
    for off in OFFS:
        pl.semaphore_signal(barrier, inc=1, device_id={"sp": moved(me, off, 1)})
    for side in sides:
        pl.semaphore_signal(barrier, inc=1, device_id={"tp": side})
    pl.semaphore_wait(barrier, len(OFFS) + 2)

    def plane(half, i):
        peer = moved(me, OFFS[i], 1)
        return pltpu.make_async_remote_copy(
            src_ref=send_ref.at[half, :, :, peer],
            dst_ref=out_ref.at[:, quarters[half], :, me],
            send_sem=ssem.at[half, i], recv_sem=rsem.at[half, i], device_id={"sp": peer},
        )

    def forward(way, i, src):
        return pltpu.make_async_remote_copy(
            src_ref=out_ref.at[:, quarters[0], :, src],
            dst_ref=out_ref.at[:, quarters[0], :, src],
            send_sem=fsem.at[way, i], recv_sem=gsem.at[way, i], device_id={"tp": sides[way]},
        )

    own = [
        pltpu.make_async_copy(
            send_ref.at[half, :, :, me], out_ref.at[:, quarters[half], :, me], lsem.at[half]
        )
        for half in range(2)
    ]
    for half in range(2):
        own[half].start()
    for half in range(2):
        for i in range(len(OFFS)):
            plane(half, i).start()
    own[0].wait()
    for way in range(2):
        forward(way, len(OFFS), me).start()

    lower = lower_mask()
    cum = dot(jnp.where(lower, 1.0, 0.0), decay_ref[...], NN, lax.Precision.HIGHEST)
    total = cum[TOK - 1 : TOK]
    for h in range(2):
        total_ref[h] = jnp.broadcast_to(jnp.exp(total[:, h * DK : (h + 1) * DK]), (8, DK))
    scales = (
        jnp.exp(cum - 0.5 * total), jnp.exp(0.5 * total - cum), jnp.exp(cum), jnp.exp(total - cum)
    )
    for i, scale in enumerate(scales):
        scale_ref[i] = scale
        scaled_ref[0, i] = (q_ref[...].astype(F32) * scale).astype(BF16)
        scaled_ref[1, i] = (k_ref[...].astype(F32) * scale).astype(BF16)
    for h in range(2):
        c = pl.ds(h * DK, DK)
        v = v_ref[:, pl.ds(h * DV, DV)]
        fwd = dot(scaled_ref[0, RISE, :, c], scaled_ref[1, FALL, :, c], NT)
        bwd = dot(scaled_ref[0, FALL, :, c], scaled_ref[1, RISE, :, c], NT)
        score_ref[h] = (jnp.where(lower, fwd, bwd) * SIGMA).astype(BF16)
        for i, kind in enumerate((TAIL, HEAD)):
            kv = dot(v, scaled_ref[1, kind, :, c], TN)
            kv_ref[i, h] = kv
            kvb_ref[i, pl.ds(h * DV, DV)] = kv.astype(BF16)

    for i, off in enumerate(OFFS):
        plane(0, i).wait_recv()
        for way in range(2):
            forward(way, i, moved(me, off, -1)).start()
    own[1].wait()
    for i in range(len(OFFS)):
        plane(1, i).wait_recv()
    for i in range(len(OFFS)):
        plane(0, i).wait_send()
        plane(1, i).wait_send()
    for i in range(len(OFFS) + 1):
        src = me if i == len(OFFS) else moved(me, OFFS[i], -1)
        for way in range(2):
            forward(way, i, src).wait()


def dispatch(send, q, k, v, decay):
    n = len(OFFS)
    return pl.pallas_call(
        dispatch_kernel,
        name="dispatch",
        out_shape=(
            jax.ShapeDtypeStruct((2, TP, 3, SP, 8, QW), BF16),
            jax.ShapeDtypeStruct((4, TOK, 2 * DK), F32),
            jax.ShapeDtypeStruct((2, 4, TOK, 2 * DK), BF16),
            jax.ShapeDtypeStruct((2, TOK, TOK), BF16),
            jax.ShapeDtypeStruct((2, 2, DV, DK), F32),
            jax.ShapeDtypeStruct((2, 2 * DV, DK), BF16),
            jax.ShapeDtypeStruct((2, 8, DK), F32),
        ),
        in_specs=[pl.BlockSpec(memory_space=VM)] * 5,
        out_specs=(pl.BlockSpec(memory_space=VM),) * 7,
        scratch_shapes=[
            pltpu.SemaphoreType.DMA((2, n)),
            pltpu.SemaphoreType.DMA((2, n)),
            pltpu.SemaphoreType.DMA((2, n + 1)),
            pltpu.SemaphoreType.DMA((2, n + 1)),
            pltpu.SemaphoreType.DMA((2,)),
        ],
        compiler_params=pltpu.CompilerParams(
            collective_id=1, has_side_effects=True, vmem_limit_bytes=32 << 20
        ),
    )(send, q, k, v, decay)


def expert_kernel(rows_ref, gate_ref, up_ref, down_ref, part_ref, act_ref, dg_ref, du_ref):
    for e in range(2):
        rows = pl.ds(256 * e, 512)
        pre_gate = pre_up = d_act = None
        for q in range(TP):
            cols = pl.ds(q * QW, QW)
            x, w = rows_ref[0, q, rows], rows_ref[1, q, rows]
            terms = (
                dot(x, gate_ref[e, cols], NN),
                dot(x, up_ref[e, cols], NN),
                dot(w, down_ref[e, :, cols], NT),
            )
            if q == 0:
                pre_gate, pre_up, d_act = terms
            else:
                pre_gate, pre_up, d_act = pre_gate + terms[0], pre_up + terms[1], d_act + terms[2]
        row = lax.broadcasted_iota(jnp.int32, (512, 256), 0)
        if e == 0:
            mine = (row < 256) | ((row & 7) < 4)
        else:
            mine = (row >= 256) | ((row & 7) >= 4)
        sig = jax.nn.sigmoid(pre_gate)
        silu = pre_gate * sig
        act_ref[e] = jnp.where(mine, silu * pre_up, 0.0).astype(BF16)
        dg = jnp.where(mine, d_act * pre_up * sig * (1.0 + pre_gate * (1.0 - sig)), 0.0).astype(BF16)
        du = jnp.where(mine, d_act * silu, 0.0).astype(BF16)
        dg_ref[e] = dg
        du_ref[e] = du
        for q in range(TP):
            cols = pl.ds(q * QW, QW)
            part = dot(dg, gate_ref[e, cols], NT) + dot(du, up_ref[e, cols], NT)
            if e == 0:
                part_ref[q, 0:512] = part.astype(BF16)
            else:
                part_ref[q, 256:512] = (part_ref[q, 256:512].astype(F32) + part[:256]).astype(BF16)
                part_ref[q, 512:768] = part[256:].astype(BF16)


def experts(rows, gate, up, down):
    hidden = jax.ShapeDtypeStruct((2, 512, 256), BF16)
    return pl.pallas_call(
        expert_kernel,
        name="experts",
        out_shape=(jax.ShapeDtypeStruct((TP, 24 * SP, QW), BF16), hidden, hidden, hidden),
        in_specs=[pl.BlockSpec(memory_space=VM)] * 4,
        out_specs=(pl.BlockSpec(memory_space=VM),) * 4,
        compiler_params=pltpu.CompilerParams(vmem_limit_bytes=48 << 20),
    )(rows, gate, up, down)


def weight_grad_kernel(rows_ref, act_ref, dg_ref, du_ref, gg_ref, gu_ref, gd_ref):
    rows = pl.ds(pl.multiple_of(pl.program_id(1) * 256, 256), 512)
    x, w = rows_ref[0, 0, rows], rows_ref[1, 0, rows]
    gg_ref[0] = dot(x, dg_ref[0], TN)
    gu_ref[0] = dot(x, du_ref[0], TN)
    gd_ref[0] = dot(act_ref[0], w, TN)


def weight_grads(rows, act, dg, du):
    hidden = pl.BlockSpec((1, 512, 256), lambda q, e: (e, 0, 0))
    wide = pl.BlockSpec((1, QW, 256), lambda q, e: (e, q, 0))
    return pl.pallas_call(
        weight_grad_kernel,
        name="weight_grads",
        grid=(TP, 2),
        out_shape=(
            jax.ShapeDtypeStruct((2, 2048, 256), F32),
            jax.ShapeDtypeStruct((2, 2048, 256), F32),
            jax.ShapeDtypeStruct((2, 256, 2048), F32),
        ),
        in_specs=[
            pl.BlockSpec((2, 1, 24 * SP, QW), lambda q, e: (0, q, 0, 0)), hidden, hidden, hidden,
        ],
        out_specs=(wide, wide, pl.BlockSpec((1, 256, QW), lambda q, e: (e, 0, q))),
        compiler_params=pltpu.CompilerParams(vmem_limit_bytes=48 << 20),
    )(rows, act, dg, du)


def give_back_kernel(
    part_ref, place_ref, cot_ref, kvb_ref, total_ref,
    tg_ref, carry_ref, decs_ref,
    side_ref, sum_ref, back_ref, half_ref, half_got_ref, first_ref, second_ref,
    xs, xr, ps, pr, ks, kr, ds_, dr, cs, cr, hs, hr, ts, tr, lsem,
):
    me, mx = lax.axis_index("sp"), lax.axis_index("tp")
    n = len(OFFS)
    xs_dev = tuple(lax.rem(mx + d, TP) for d in (1, 3))
    across = lax.rem(mx + 2, TP)
    barrier = pltpu.get_barrier_semaphore()
    for off in OFFS:
        pl.semaphore_signal(barrier, inc=1, device_id={"sp": moved(me, off, 1)})
    for d in (1, 2, 3):
        pl.semaphore_signal(barrier, inc=1, device_id={"tp": lax.rem(mx + d, TP)})
    pl.semaphore_wait(barrier, n + 3)

    def peer(i):
        return me if i == n else moved(me, OFFS[i], 1)

    def states_out(i):
        to = peer(i)
        return (
            pltpu.make_async_remote_copy(
                src_ref=kvb_ref.at[:, to], dst_ref=first_ref.at[me],
                send_sem=ks.at[i], recv_sem=kr.at[i], device_id={"sp": to},
            ),
            pltpu.make_async_remote_copy(
                src_ref=total_ref.at[to // (SP // 2)], dst_ref=decs_ref.at[me],
                send_sem=ds_.at[i], recv_sem=dr.at[i], device_id={"sp": to},
            ),
        )

    def states_back(i):
        to = peer(i)
        return pltpu.make_async_remote_copy(
            src_ref=second_ref.at[to], dst_ref=carry_ref.at[:, me],
            send_sem=cs.at[i], recv_sem=cr.at[i], device_id={"sp": to},
        )

    def aside(way, i):
        to = peer(i)
        return pltpu.make_async_remote_copy(
            src_ref=part_ref.at[xs_dev[way], :, to], dst_ref=side_ref.at[way, :, to],
            send_sem=xs.at[way, i], recv_sem=xr.at[way, i], device_id={"tp": xs_dev[way]},
        )

    def plane(half, i):
        to = peer(i)
        src = sum_ref.at[:, to] if half == 0 else part_ref.at[across, :, to]
        return pltpu.make_async_remote_copy(
            src_ref=src, dst_ref=back_ref.at[half, :, me],
            send_sem=ps.at[half, i], recv_sem=pr.at[half, i], device_id={"sp": to},
        )

    own = (
        pltpu.make_async_copy(kvb_ref.at[:, me], first_ref.at[me], lsem.at[0]),
        pltpu.make_async_copy(total_ref.at[me // (SP // 2)], decs_ref.at[me], lsem.at[1]),
        pltpu.make_async_copy(part_ref.at[across, :, me], back_ref.at[1, :, me], lsem.at[2]),
    )
    for copy in own:
        copy.start()
    for i in range(n):
        for copy in states_out(i):
            copy.start()
    for i in range(n + 1):
        for way in range(2):
            aside(way, i).start()
    for i in range(n):
        plane(1, i).start()

    own[0].wait()
    own[1].wait()
    for i in range(n):
        for copy in states_out(i):
            copy.wait()
    scan_into(first_ref, decs_ref, second_ref)
    for i in range(n):
        states_back(i).start()
    carry_ref[:, me] = second_ref[me]

    for i in range(n + 1):
        for way in range(2):
            aside(way, i).wait()
        to = peer(i)
        total = (
            part_ref[mx, :, to].astype(F32)
            + side_ref[0, :, to].astype(F32) + side_ref[1, :, to].astype(F32)
        ).astype(BF16)
        if i < n:
            sum_ref[:, to] = total
            if i > 0:
                plane(0, i - 1).start()
        else:
            plane(0, n - 1).start()
            back_ref[0, :, me] = total

    own[2].wait()
    for i in range(n):
        plane(1, i).wait()
    place = place_ref[...]
    half_ref[...] = dot(place, back_ref[1].reshape(24 * SP, QW), TN).astype(BF16)
    over = pltpu.make_async_remote_copy(
        src_ref=half_ref, dst_ref=half_got_ref, send_sem=hs, recv_sem=hr, device_id={"tp": across}
    )
    for i in range(n):
        states_back(i).wait()
    over.start()
    for i in range(n):
        plane(0, i).wait()
    cols = pl.ds(pl.multiple_of(mx * QW, QW), QW)
    token = cot_ref[:, cols].astype(F32) + dot(place, back_ref[0].reshape(24 * SP, QW), TN)
    over.wait()
    tg_ref[mx] = (token + half_got_ref[...].astype(F32)).astype(BF16)
    spread = [
        pltpu.make_async_remote_copy(
            src_ref=tg_ref.at[mx], dst_ref=tg_ref.at[mx],
            send_sem=ts.at[d], recv_sem=tr.at[d], device_id={"tp": lax.rem(mx + d + 1, TP)},
        )
        for d in range(3)
    ]
    for copy in spread:
        copy.start()
    for copy in spread:
        copy.wait()


def scan_into(got_ref, decs_ref, out_ref):
    for state, order in ((0, range(SP)), (1, range(SP - 1, -1, -1))):
        acc = jnp.zeros((16, DK), F32)
        for s in order:
            out_ref[s, state] = acc.astype(BF16)
            acc = decs_ref[s, 0:1] * acc + got_ref[s, state].astype(F32)


def give_back(part, place, cot, kvb, total):
    n = len(OFFS)
    dma = pltpu.SemaphoreType.DMA
    return pl.pallas_call(
        give_back_kernel,
        name="give_back",
        out_shape=(
            jax.ShapeDtypeStruct((TP, TOK, QW), BF16),
            jax.ShapeDtypeStruct((2, SP, 16, DK), BF16),
            jax.ShapeDtypeStruct((SP, 8, DK), F32),
        ),
        in_specs=[pl.BlockSpec(memory_space=VM)] * 5,
        out_specs=(pl.BlockSpec(memory_space=VM),) * 3,
        scratch_shapes=[
            VM((2, 3, SP, 8, QW), BF16),
            VM((3, SP, 8, QW), BF16),
            VM((2, 3, SP, 8, QW), BF16),
            VM((TOK, QW), BF16),
            VM((TOK, QW), BF16),
            VM((SP, 2, 16, DK), BF16),
            VM((SP, 2, 16, DK), BF16),
            dma((2, n + 1)), dma((2, n + 1)), dma((2, n)), dma((2, n)),
            dma((n,)), dma((n,)), dma((n,)), dma((n,)), dma((n,)), dma((n,)),
            dma, dma, dma((3,)), dma((3,)), dma((3,)),
        ],
        compiler_params=pltpu.CompilerParams(
            collective_id=2, has_side_effects=True, vmem_limit_bytes=32 << 20
        ),
    )(part, place, cot, kvb, total)


def attention_kernel(
    tg_ref, proj_ref, mixed_ref, q_ref, k_ref, v_ref,
    scale_ref, scaled_ref, score_ref, kv_ref, kvc_ref, total_ref, decs_ref,
    gp_ref, gq_ref, gk_ref, gv_ref, gd_ref,
    gf_ref, qo_ref, qob_ref, first_ref, second_ref, carry_ref, local_ref,
    keep_ref, give_ref, got_ref, share_ref, gather_ref,
    qs, qr, cs, cr, ms, mr, gs, gr, lsem,
):
    me = lax.axis_index("sp")
    n = len(OFFS)
    core = lax.rem(me, 2)
    chip = me // 2
    barrier = pltpu.get_barrier_semaphore()
    for off in OFFS:
        pl.semaphore_signal(barrier, inc=1, device_id={"sp": moved(me, off, 1)})

    def peer(i):
        return moved(me, OFFS[i], 1)

    def states_out(i):
        to = peer(i)
        return pltpu.make_async_remote_copy(
            src_ref=qob_ref.at[:, to], dst_ref=first_ref.at[me],
            send_sem=qs.at[i], recv_sem=qr.at[i], device_id={"sp": to},
        )

    def states_back(i):
        to = peer(i)
        return pltpu.make_async_remote_copy(
            src_ref=second_ref.at[to], dst_ref=carry_ref.at[:, me],
            send_sem=cs.at[i], recv_sem=cr.at[i], device_id={"sp": to},
        )

    chips = [i for i, off in enumerate(OFFS) if off[2] == 0]

    def share(j):
        to = peer(chips[j])
        return pltpu.make_async_remote_copy(
            src_ref=share_ref.at[to // 2], dst_ref=gather_ref.at[chip],
            send_sem=gs.at[j], recv_sem=gr.at[j], device_id={"sp": to},
        )

    grad = None
    for p in range(TP):
        term = dot(tg_ref[p], proj_ref[:, pl.ds(p * QW, QW)], NT)
        grad = term if grad is None else grad + term
    gf_ref[...] = grad.astype(BF16)
    for h in range(2):
        gf = gf_ref[:, pl.ds(h * DV, DV)]
        c = pl.ds(h * DK, DK)
        for i, kind in enumerate((TAIL, HEAD)):
            qo = dot(gf, scaled_ref[0, kind, :, c], TN)
            qo_ref[i, h] = qo
            qob_ref[i, pl.ds(h * SP // 2, SP // 2)] = qo.astype(BF16).reshape(SP // 2, 16, DK)
    pl.semaphore_wait(barrier, n)
    for i in range(n):
        states_out(i).start()
    first_ref[me] = qob_ref[:, me]

    mixed = mixed_ref[...]
    for p in range(TP):
        part = dot(tg_ref[p], mixed, TN).reshape(4, 2, 64, QW)
        for b in range(4):
            keep_ref[p * 4 + b] = jnp.where(core == 0, part[b, 0], part[b, 1])
            give_ref[p * 4 + b] = jnp.where(core == 0, part[b, 1], part[b, 0]).astype(BF16)
    swap = pltpu.make_async_remote_copy(
        src_ref=give_ref, dst_ref=got_ref, send_sem=ms, recv_sem=mr, device_id={"sp": peer(0)}
    )
    swap.start()

    lower = lower_mask()
    for h in range(2):
        c = pl.ds(h * DK, DK)
        gf, v = gf_ref[:, pl.ds(h * DV, DV)], v_ref[:, pl.ds(h * DV, DV)]
        pair = dot(gf, v, NT)
        fwd, bwd = jnp.where(lower, pair, 0.0).astype(BF16), jnp.where(lower, 0.0, pair).astype(BF16)
        rise, fall = scale_ref[RISE, :, c], scale_ref[FALL, :, c]
        local_ref[0, :, c] = rise * dot(fwd, scaled_ref[1, FALL, :, c], NN)
        local_ref[1, :, c] = fall * dot(bwd, scaled_ref[1, RISE, :, c], NN)
        local_ref[2, :, c] = fall * dot(fwd, scaled_ref[0, RISE, :, c], TN)
        local_ref[3, :, c] = rise * dot(bwd, scaled_ref[0, FALL, :, c], TN)
        gv_ref[:, pl.ds(h * DV, DV)] = dot(score_ref[h], gf, TN)

    for i in range(n):
        states_out(i).wait()
    scan_into(first_ref, decs_ref, second_ref)
    for i in range(n):
        states_back(i).start()
    carry_ref[:, me] = second_ref[me]
    swap.wait()
    for m in range(SP // 2):
        share_ref[m] = (keep_ref[m] + got_ref[m].astype(F32)).astype(BF16)
    for i in range(n):
        states_back(i).wait()
    for j in range(len(chips)):
        share(j).start()

    for h in range(2):
        c = pl.ds(h * DK, DK)
        rows = pl.ds(h * SP // 2, SP // 2)
        vcols = pl.ds(h * DV, DV)
        gf, v = gf_ref[:, vcols], v_ref[:, vcols]
        qo_low, qo_high = carry_ref[0, rows].reshape(DV, DK), carry_ref[1, rows].reshape(DV, DK)
        kv_low, kv_high = kvc_ref[0, rows].reshape(DV, DK), kvc_ref[1, rows].reshape(DV, DK)
        head, tail = scale_ref[HEAD, :, c], scale_ref[TAIL, :, c]
        q_fwd = local_ref[0, :, c] + head * dot(gf, kv_low, NN)
        q_bwd = local_ref[1, :, c] + tail * dot(gf, kv_high, NN)
        k_fwd = local_ref[2, :, c] + tail * dot(v, qo_high, NN)
        k_bwd = local_ref[3, :, c] + head * dot(v, qo_low, NN)
        gq_ref[:, c] = SIGMA * (q_fwd + q_bwd)
        gk_ref[:, c] = SIGMA * (k_fwd + k_bwd)
        gv_ref[:, vcols] = gv_ref[:, vcols] + SIGMA * (
            dot(scaled_ref[1, TAIL, :, c], qo_high, NT) + dot(scaled_ref[1, HEAD, :, c], qo_low, NT)
        )
        grad_cum = SIGMA * (
            q_ref[:, c].astype(F32) * (q_fwd - q_bwd) - k_ref[:, c].astype(F32) * (k_fwd - k_bwd)
        )
        decay = total_ref[h, 0:1]
        beyond = SIGMA * jnp.sum(
            (decay * kv_low.astype(F32) + kv_ref[0, h]) * qo_high.astype(F32)
            + (decay * qo_low.astype(F32) + qo_ref[0, h]) * kv_high.astype(F32),
            axis=0, keepdims=True,
        )
        upper = jnp.where(
            lax.broadcasted_iota(jnp.int32, (TOK, TOK), 0)
            <= lax.broadcasted_iota(jnp.int32, (TOK, TOK), 1), 1.0, 0.0,
        )
        gd_ref[:, c] = dot(upper, grad_cum, NN, lax.Precision.HIGHEST) + beyond

    for j in range(len(chips)):
        share(j).wait()
    total = share_ref[chip].astype(F32)
    for j in range(len(chips)):
        dy, dz, _ = OFFS[chips[j]]
        total = total + gather_ref[moved(me, (dy, dz, 0), -1) // 2].astype(F32)
    gp_ref[...] = total


def attention(*operands):
    n = len(OFFS)
    dma = pltpu.SemaphoreType.DMA
    small = jax.ShapeDtypeStruct((TOK, 2 * DK), F32)
    return pl.pallas_call(
        attention_kernel,
        name="attention",
        out_shape=(
            jax.ShapeDtypeStruct((64, QW), F32), small, small,
            jax.ShapeDtypeStruct((TOK, 2 * DV), F32), small,
        ),
        in_specs=[pl.BlockSpec(memory_space=VM)] * len(operands),
        out_specs=(pl.BlockSpec(memory_space=VM),) * 5,
        scratch_shapes=[
            VM((TOK, 2 * DV), BF16),
            VM((2, 2, DV, DK), F32),
            VM((2, SP, 16, DK), BF16),
            VM((SP, 2, 16, DK), BF16),
            VM((SP, 2, 16, DK), BF16),
            VM((2, SP, 16, DK), BF16),
            VM((4, TOK, 2 * DK), F32),
            VM((SP // 2, 64, QW), F32),
            VM((SP // 2, 64, QW), BF16),
            VM((SP // 2, 64, QW), BF16),
            VM((SP // 2, 64, QW), BF16),
            VM((SP // 2, 64, QW), BF16),
            dma((n,)), dma((n,)), dma((n,)), dma((n,)), dma, dma, dma((15,)), dma((15,)), dma,
        ],
        compiler_params=pltpu.CompilerParams(
            collective_id=3, has_side_effects=True, vmem_limit_bytes=40 << 20
        ),
    )(*operands)


def body(
    queries, key_vectors, values_in, log_decay, mixed_heads, out_proj, layer_input, cotangent,
    routes, route_weight, gate_weight, up_weight, down_weight,
):
    place, send = prep(routes.T, route_weight.T, layer_input, cotangent)
    got, scale, scaled, score, kv, kvb, total = dispatch(
        send.reshape(2, 2, 3, SP, 8, QW), queries, key_vectors, values_in, log_decay
    )
    got = got.reshape(2, TP, 24 * SP, QW)
    part, act, dg, du = experts(got, gate_weight, up_weight, down_weight)
    tg, carry, decs = give_back(
        part.reshape(TP, 3, SP, 8, QW), place, cotangent, kvb.reshape(2, SP, 16, DK), total
    )
    grad_gate, grad_up, grad_down = weight_grads(got, act, dg, du)
    grad_proj, grad_q, grad_k, grad_v, grad_decay = attention(
        tg, out_proj, mixed_heads, queries, key_vectors, values_in,
        scale, scaled, score, kv, carry, total, decs,
    )
    return grad_gate, grad_up, grad_down, grad_proj, grad_q, grad_k, grad_v, grad_decay


def solution(mesh):
    return jax.shard_map(
        body,
        mesh=mesh,
        in_specs=(
            P("sp", "tp"), P("sp", "tp"), P("sp", "tp"), P("sp", "tp"), P("sp", "tp"),
            P("tp", None), P("sp", None), P("sp", None), P("sp", None), P("sp", None),
            P("sp", None, "tp"), P("sp", None, "tp"), P("sp", "tp", None),
        ),
        out_specs=(
            P("sp", None, "tp"), P("sp", None, "tp"), P("sp", "tp", None),
            P("sp", "tp"), P("sp", "tp"), P("sp", "tp"), P("sp", "tp"), P("sp", "tp"),
        ),
        check_vma=False,
    )
```
